512 devices in a mesh: ep: 16 (over y, x), tp: 32 (over z, core).
Axes of the slice: x: 4, y: 4, z: 16, core: 2. Of those that a mesh axis runs over, the one named last changes fastest.
Arguments:
- tokens: bfloat16 [2048, 4096], P('ep', 'tp'), may hold values from -16 to 16
- routing: int32 [2048, 4], P('ep'), may hold values from 0 to 31, all different within a row; in each aligned block of 128 rows (0 to 127, 128 to 255, ...) at most 32 rows name the same one
- gate_weights: float32 [2048, 4], P('ep'), may hold values from 0.1 to 1
- w_gate: bfloat16 [32, 1024, 4096], P('ep', 'tp'), may hold values from -0.09375 to 0.09375
- w_up: bfloat16 [32, 1024, 4096], P('ep', 'tp'), may hold values from -0.09375 to 0.09375
- w_down: bfloat16 [32, 1024, 4096], P('ep', None, 'tp'), may hold values from -2 to 2
- out_gain: float32 [4096], P('tp'), may hold values from 0.1 to 1.9
Outputs:
- mixed: bfloat16 [2048, 4096], P('ep', 'tp')
The draws below stay inside these ranges and needn't reach their ends.
Inputs may be any that keep to these rules, and one draw needn't show every extreme that they name: `routing`: in each aligned block of 128 rows (the tokens of one index of ep) no expert is named by more than 32 entries, and in every draw some expert is named by exactly 32 entries of some block. The 4 entries of a row differ.
All inputs are finite; a program needn't handle non-finite values.
Results may differ from the reference program's by a relative error of at most 0.0057.
Values may be sent and summed in bfloat16 or wider, within the bound.
A program may use at most 64 MiB of HBM per device.

```python
import math
import jax
import jax.numpy as jnp
import numpy as np
from jax import lax

D = 4096
FE = 1024
TOPK = 4
EXP_DEV = 2
EXPERTS = 32
TOK_EP = 128
TOKENS = 2048
CAP = 32
N_EP = 16


def draw_tokens(key, part):
    first_key, second_key = jax.random.split(key)
    base = jnp.clip(jax.random.normal(first_key, (TOKENS, D), jnp.float32), -4.5, 4.5)
    row_factor = jnp.exp(jax.random.uniform(second_key, (TOKENS, 1), jnp.float32, -1.2, 1.2))
    return (base * row_factor).astype(jnp.bfloat16)


def draw_w_down(key, part):
    first_key, second_key = jax.random.split(jax.random.fold_in(key, 7))
    base = jnp.clip(jax.random.normal(first_key, (EXPERTS, FE, D), jnp.float32), -4.5, 4.5) * FE ** (-0.5)
    group_factor = jnp.exp(jax.random.uniform(second_key, (16,), jnp.float32, -1.1, 1.1))
    column_factor = jnp.repeat(group_factor, D // 16)
    return (base * column_factor[None, None, :]).astype(jnp.bfloat16)


def block_levels(rng, shape, shards, low, largest):
    loudness = 1.0
    for position, parts in shards:
        heights = jax.random.uniform(jax.random.fold_in(jax.random.fold_in(rng, 6), position), (parts,), jnp.float32, low / len(shards), largest / len(shards))
        loudness = loudness * jnp.repeat(jnp.exp(heights), shape[position] // parts).reshape((-1,) + (1,) * (len(shape) - 1 - position))
    return loudness


def deal_out(own_key, own, number, rows, number_of, top, bound, lean):
    order = jax.random.permutation(own_key, number_of)
    packed, usual = portions_of(number_of, rows * top, bound, lean, True), portions_of(number_of, rows * top, bound, lean, False)
    places = jnp.arange(number_of)

    def named(tallies, offset_by):
        used = int((tallies > 0).sum())
        fixed = max(1, used // 4)
        moved = fixed + (places - fixed + offset_by * (used - fixed)) % max(1, number_of - fixed)
        return jnp.zeros((number_of,), jnp.int32).at[order[jnp.where(places < fixed, places, moved)]].set(jnp.asarray(tallies, jnp.int32))

    tallies = jnp.where(number % 4 == 0, named(packed, number // 4), named(usual, number - number // 4 - 1))
    mixed = jax.random.permutation(jax.random.fold_in(own, 3), number_of)
    giver, receiver = mixed[0:number_of // 2 * 2:2], mixed[1:number_of // 2 * 2:2]
    slack = jnp.minimum(tallies[giver] - 1, bound - tallies[receiver]) // 2
    slack = jnp.where((giver == order[0]) | (receiver == order[0]) | (tallies[receiver] == 0), 0, jnp.maximum(slack, 0))
    moved = jax.random.randint(jax.random.fold_in(own, 4), (number_of // 2,), 0, 1 << 20) % (slack + 1)
    tallies = tallies.at[giver].add(-moved).at[receiver].add(moved)
    labels = jnp.searchsorted(jnp.cumsum(tallies), jnp.arange(rows * top), side="right").astype(jnp.int32)
    grid = labels.reshape(top, rows).T
    grid = grid[jax.random.permutation(jax.random.fold_in(own, 1), rows)]
    offset_by = jax.random.randint(jax.random.fold_in(own, 2), (rows, 1), 0, top)
    return jnp.take_along_axis(grid, (jnp.arange(top)[None, :] + offset_by) % top, axis=1)


def portions_of(number_of, total, bound, skew, full):
    portions = [(1 << 20) // math.isqrt(grade ** skew) + 1 for grade in range(1, number_of + 1)]
    largest = bound if full else min(bound, max(-(-total // number_of), total * portions[0] // sum(portions)))
    least = 1 if total - largest >= number_of - 1 else 0
    given, spare = [largest] + [least] * (number_of - 1), total - largest - least * (number_of - 1)
    while spare > 0:
        candidates = [i for i in range(1, number_of) if given[i] < largest] or [i for i in range(1, number_of) if given[i] < bound]
        whole, budget = sum([portions[i] for i in candidates]), spare
        for i in candidates:
            extra = min(bound - given[i], max(1, budget * portions[i] // whole), spare)
            given[i] = given[i] + extra
            spare = spare - extra
    return np.array(given)


def scatter_about(own_key, extent, scale, reach, cuts=(), kind=jnp.bfloat16):
    factor_of = block_levels(own_key, extent, cuts, -0.22, 0.18) if cuts else 1.0
    drawn = jax.random.normal(own_key, extent, jnp.float32) * scale * factor_of
    return jnp.minimum(jnp.maximum(drawn, -reach), reach).astype(kind)


def setup_inputs(seed: int = 0) -> dict:
    key_of = jax.random.split(jax.random.key(seed), 8)
    tokens = draw_tokens(jax.random.fold_in(key_of[7], 71), 0)
    routing_keys = jax.random.split(jax.random.fold_in(key_of[1], 1), TOKENS // TOK_EP)
    routing_turns = jax.random.permutation(jax.random.fold_in(key_of[1], 3), TOKENS // TOK_EP)
    routing = jax.vmap(lambda own, number: deal_out(jax.random.fold_in(key_of[1], 2), own, number, TOK_EP, EXPERTS, TOPK, CAP, 2))(routing_keys, routing_turns).reshape((TOKENS, TOPK))
    gate_weights = jnp.clip(0.1 + 0.9 * jax.random.uniform(key_of[2], (TOKENS, TOPK), jnp.float32) ** block_levels(key_of[2], (TOKENS, TOPK), ((0, 16),), -0.2, 0.2), 0.1, 1.0)
    w_gate = scatter_about(key_of[3], (EXPERTS, FE, D), D ** -0.5, 0.09375, ((0, 16), (1, 32)))
    w_up = scatter_about(key_of[4], (EXPERTS, FE, D), D ** -0.5, 0.09375, ((0, 16), (1, 32)))
    w_down = draw_w_down(jax.random.fold_in(key_of[7], 71), 0)
    out_gain = jnp.clip(1.0 + 0.18 * jax.random.normal(key_of[6], (D,), jnp.float32), 0.1, 1.9)
    return {"tokens": tokens, "routing": routing, "gate_weights": gate_weights, "w_gate": w_gate, "w_up": w_up, "w_down": w_down, "out_gain": out_gain}


norm_eps = 1e-05

def reference(tokens, routing, gate_weights, w_gate, w_up, w_down, out_gain):
    experts = EXP_DEV * N_EP
    rows_max = N_EP * CAP
    token_f = tokens.astype(jnp.float32)
    row_scale = lax.rsqrt(lax.optimization_barrier(jnp.mean(token_f * token_f, axis=1)) + norm_eps)
    flat_route = routing.reshape(-1).astype(jnp.int32)
    entry_count = flat_route.shape[0]
    expert_ids = jnp.arange(experts, dtype=jnp.int32)
    hit_table = (flat_route[:, None] == expert_ids[None, :]).astype(jnp.int32)
    running = jnp.cumsum(hit_table, axis=0).astype(jnp.int32) - hit_table
    slot_rank = lax.optimization_barrier(jnp.sum(running * hit_table, axis=1)).astype(jnp.int32)
    owner = (jnp.arange(entry_count, dtype=jnp.int32) // TOPK).astype(jnp.int32)

    def one_expert(inputs):
        expert_id, gate_mat, up_mat, down_mat = inputs
        target = jnp.where(flat_route == expert_id, slot_rank, rows_max).astype(jnp.int32)
        row_ids = jnp.zeros((rows_max,), jnp.int32).at[target].set(owner, mode='drop')
        picked_rows = tokens[row_ids]
        scale_rows = row_scale[row_ids][:, None]
        gate_pre = jnp.dot(picked_rows, gate_mat.T, preferred_element_type=jnp.float32) * scale_rows
        up_pre = jnp.dot(picked_rows, up_mat.T, preferred_element_type=jnp.float32) * scale_rows
        hidden = (jax.nn.silu(gate_pre) * up_pre).astype(jnp.bfloat16)
        return jnp.dot(hidden, down_mat, preferred_element_type=jnp.float32).astype(jnp.bfloat16)
    expert_outs = lax.map(one_expert, (expert_ids, w_gate, w_up, w_down))
    chosen = expert_outs[flat_route, slot_rank].astype(jnp.float32).reshape(TOKENS, TOPK, D)
    combined = lax.optimization_barrier(jnp.sum(chosen * gate_weights[:, :, None], axis=1))
    final_scale = lax.rsqrt(lax.optimization_barrier(jnp.mean(combined * combined, axis=1)) + norm_eps)
    return (combined * final_scale[:, None] * out_gain[None, :]).astype(jnp.bfloat16)
```

```python
import functools
import jax
import jax.numpy as jnp
from jax import lax
from jax.experimental import pallas as pl
from jax.experimental.pallas import tpu as pltpu
from jax.sharding import PartitionSpec as P

EXP_DEV = 2
CAP = 32
NORM_EPS = 1e-05
MESH = pl.DeviceIdType.MESH
F32 = jnp.float32
BF16 = jnp.bfloat16


def dot(a, b, dims):
    return lax.dot_general(a, b, (dims, ((), ())), preferred_element_type=F32)


def layer_kernel(
    n_ep, n_z, tok_ref, rt_ref, gw_ref, wg_ref, wu_ref, wd_ref, gain_ref, out_ref,
    outgoing, combine_w, x_all, w_all, d_all, acc, squares, h_all, o_acc, back, y_all, norm_all,
    w_sem, w_send, w_recv, d_send, d_recv, local_sem,
    x_send, x_recv, h_send, h_recv, r_send, r_recv, n_send, n_recv,
):
    ep = lax.axis_index("ep")
    tp = lax.axis_index("tp")
    z, c = tp // 2, tp % 2
    other = 1 - c
    partner = 2 * z + other
    above, below = (z + 1) % n_z, (z + n_z - 1) % n_z
    n_exp = EXP_DEV * n_ep
    n_tp = 2 * n_z
    tok_rows, width = tok_ref.shape
    half = n_z // 2
    rows = n_ep * CAP

    barrier = pltpu.get_barrier_semaphore()

    def greet(j, carry):
        p_to, c_to = (ep + j // 2) % n_ep, (c + j % 2) % 2
        pl.semaphore_signal(barrier, inc=1, device_id=(p_to, 2 * z + c_to), device_id_type=MESH)
        return carry

    lax.fori_loop(1, 2 * n_ep, greet, 0)
    pl.semaphore_signal(barrier, inc=1, device_id=(ep, 2 * above + c), device_id_type=MESH)
    pl.semaphore_signal(barrier, inc=1, device_id=(ep, 2 * below + c), device_id_type=MESH)

    own_w = [
        pltpu.make_async_copy(wg_ref.at[c], w_all.at[0, c], w_sem.at[0]),
        pltpu.make_async_copy(wu_ref.at[c], w_all.at[1, c], w_sem.at[1]),
        pltpu.make_async_copy(wd_ref.at[c], d_all.at[:, pl.ds(pl.multiple_of(c * width, width), width)], w_sem.at[2]),
    ]
    for copy in own_w:
        copy.start()

    rt = rt_ref[...]
    expert_ids = lax.broadcasted_iota(jnp.int32, (n_exp, tok_rows), 0)
    hits = [expert_ids == rt[k : k + 1, :] for k in range(rt.shape[0])]
    hit = functools.reduce(jnp.logical_or, hits)
    earlier = (
        lax.broadcasted_iota(jnp.int32, (tok_rows, tok_rows), 0)
        < lax.broadcasted_iota(jnp.int32, (tok_rows, tok_rows), 1)
    )
    rank = dot(
        jnp.where(hit, 1.0, 0.0).astype(BF16), jnp.where(earlier, 1.0, 0.0).astype(BF16), ((1,), (0,))
    )
    rank = jnp.where(hit, rank, -1.0)
    slot_ids = lax.broadcasted_iota(jnp.int32, (n_exp, CAP, tok_rows), 1).astype(F32)
    chosen = slot_ids == rank[:, None, :]
    select = jnp.where(chosen, 1.0, 0.0).astype(BF16).reshape(n_exp * CAP, tok_rows)
    outgoing[...] = dot(select, tok_ref[...], ((1,), (0,))).astype(BF16).reshape(n_exp, CAP, width)

    pl.semaphore_wait(barrier, 2 * n_ep - 1 + 2)

    def spread(j):
        p_to, c_to = (ep + j // 2) % n_ep, (c + j % 2) % 2
        return pltpu.make_async_remote_copy(
            src_ref=outgoing.at[2 * p_to + c_to],
            dst_ref=x_all.at[z, c, pl.ds(pl.multiple_of(ep * CAP, CAP), CAP)],
            send_sem=d_send.at[j],
            recv_sem=d_recv.at[j],
            device_id=(p_to, 2 * z + c_to),
            device_id_type=MESH,
        )

    def landed(j):
        p_from, c_from = (ep + n_ep - j // 2) % n_ep, (c + j % 2) % 2
        return pltpu.make_async_remote_copy(
            src_ref=outgoing.at[0],
            dst_ref=x_all.at[z, c_from, pl.ds(pl.multiple_of(p_from * CAP, CAP), CAP)],
            send_sem=d_send.at[j],
            recv_sem=d_recv.at[j],
            device_id=(p_from, 2 * z + c_from),
            device_id_type=MESH,
        )

    def each(lo, hi, act):
        def step(j, carry):
            act(j)
            return carry

        lax.fori_loop(lo, hi, step, 0)

    each(1, 2 * n_ep, lambda j: spread(j).start())
    own_x = pltpu.make_async_copy(
        outgoing.at[2 * ep + c], x_all.at[z, c, pl.ds(pl.multiple_of(ep * CAP, CAP), CAP)], local_sem.at[0]
    )
    own_x.start()

    pair_w = [
        pltpu.make_async_remote_copy(
            src_ref=src, dst_ref=dst, send_sem=w_send.at[i], recv_sem=w_recv.at[i],
            device_id=(ep, partner), device_id_type=MESH,
        )
        for i, (src, dst) in enumerate((
            (wg_ref.at[other], w_all.at[0, c]),
            (wu_ref.at[other], w_all.at[1, c]),
            (wd_ref.at[other], d_all.at[:, pl.ds(pl.multiple_of(c * width, width), width)]),
        ))
    ]
    pair_in = [
        pltpu.make_async_remote_copy(
            src_ref=src, dst_ref=dst, send_sem=w_send.at[i], recv_sem=w_recv.at[i],
            device_id=(ep, partner), device_id_type=MESH,
        )
        for i, (src, dst) in enumerate((
            (wg_ref.at[other], w_all.at[0, other]),
            (wu_ref.at[other], w_all.at[1, other]),
            (wd_ref.at[other], d_all.at[:, pl.ds(pl.multiple_of(other * width, width), width)]),
        ))
    ]
    for copy in pair_w:
        copy.start()

    gate_of = functools.reduce(
        jnp.add, [jnp.where(hits[k], gw_ref[k : k + 1, :], 0.0) for k in range(rt.shape[0])]
    )
    weight = jnp.where(chosen, gate_of[:, None, :], 0.0).reshape(n_exp * CAP, tok_rows).T
    weight_hi = weight.astype(BF16)
    combine_w[0] = weight_hi
    combine_w[1] = (weight - weight_hi.astype(F32)).astype(BF16)

    acc[...] = jnp.zeros_like(acc)
    squares[...] = jnp.zeros_like(squares)
    o_acc[...] = jnp.zeros_like(o_acc)

    def ring(buf, send, recv, use):
        def hop(way, s, ch):
            block = (z + n_z - s) % n_z if way == 0 else (z + s) % n_z
            to = above if way == 0 else below
            return pltpu.make_async_remote_copy(
                src_ref=buf.at[block, ch], dst_ref=buf.at[block, ch],
                send_sem=send.at[way, s, ch], recv_sem=recv.at[way, s, ch],
                device_id=(ep, 2 * to + c), device_id_type=MESH,
            )

        def came(way, s, ch):
            block = (z + n_z - s) % n_z if way == 0 else (z + s) % n_z
            return pltpu.make_async_remote_copy(
                src_ref=buf.at[block, ch], dst_ref=buf.at[block, ch],
                send_sem=send.at[way, s - 1, ch], recv_sem=recv.at[way, s - 1, ch],
                device_id=(ep, 2 * (below if way == 0 else above) + c), device_id_type=MESH,
            )

        order = ((0, 0), (1, 1), (0, 1), (1, 0))
        for way, ch in order:
            hop(way, 0, ch).start()
        use(z, 0)
        use(z, 1)

        def step(s):
            for way, ch in order:
                came(way, s, ch).wait_recv()
                hop(way, s, ch).start()
            for way, ch in order:
                use((z + n_z - s) % n_z if way == 0 else (z + s) % n_z, ch)

        each(1, half - 1, step)
        s = half - 1
        for way, ch in order:
            came(way, s, ch).wait_recv()
            if way == ch:
                hop(way, s, ch).start()
        for way, ch in order:
            use((z + n_z - s) % n_z if way == 0 else (z + s) % n_z, ch)
        for way in (0, 1):
            came(way, half, way).wait_recv()
            use((z + half) % n_z, way)

        def sent():
            def done(s):
                for way, ch in order:
                    hop(way, s, ch).wait_send()

            each(0, half - 1, done)
            for way in (0, 1):
                hop(way, half - 1, way).wait_send()

        return sent

    own_x.wait()
    each(1, 2 * n_ep, lambda j: landed(j).wait_recv())
    for copy in own_w:
        copy.wait()
    for copy in pair_in:
        copy.wait_recv()

    n_hid = 2 * w_all.shape[2]

    def project(block, ch):
        x = x_all[block, ch]
        column = pl.multiple_of((2 * block + ch) * width, width)
        w = w_all[:, :, :, pl.ds(column, width)].reshape(2 * n_hid, width)
        acc[...] += dot(w, x, ((1,), (1,)))
        x = x.astype(F32)
        squares[...] += x * x

    x_sent = ring(x_all, x_send, x_recv, project)

    features = n_tp * width
    square_sum = jnp.sum(squares[...].T, axis=0, keepdims=True)
    row_scale = lax.rsqrt(square_sum * (1.0 / features) + NORM_EPS)
    gate = acc[0:n_hid, :] * row_scale
    up = acc[n_hid : 2 * n_hid, :] * row_scale
    hidden = (gate / (1.0 + jnp.exp(-gate)) * up).astype(BF16)
    part = rows // 2
    for i in range(2):
        h_all[z, i] = hidden[:, i * part : (i + 1) * part]

    def down(block, ch):
        w = d_all[pl.ds(pl.multiple_of(block * n_hid, n_hid), n_hid), :]
        o_acc[ch] += dot(h_all[block, ch], w, ((0,), (0,)))

    h_sent = ring(h_all, h_send, h_recv, down)

    for i in range(2):
        for h in range(2):
            back[h, i * (n_ep // 2) : (i + 1) * (n_ep // 2)] = (
                o_acc[i, :, h * width : (h + 1) * width].astype(BF16).reshape(n_ep // 2, CAP, width)
            )

    def give(j):
        p_to, c_to = (ep + j // 2) % n_ep, (c + j % 2) % 2
        return pltpu.make_async_remote_copy(
            src_ref=back.at[c_to, p_to], dst_ref=y_all.at[2 * ep + c],
            send_sem=r_send.at[j], recv_sem=r_recv.at[j],
            device_id=(p_to, 2 * z + c_to), device_id_type=MESH,
        )

    def got(j):
        p_from, c_from = (ep + n_ep - j // 2) % n_ep, (c + j % 2) % 2
        return pltpu.make_async_remote_copy(
            src_ref=back.at[0, 0], dst_ref=y_all.at[2 * p_from + c_from],
            send_sem=r_send.at[j], recv_sem=r_recv.at[j],
            device_id=(p_from, 2 * z + c_from), device_id_type=MESH,
        )

    each(1, 2 * n_ep, lambda j: give(j).start())
    own_y = pltpu.make_async_copy(back.at[c, ep], y_all.at[2 * ep + c], local_sem.at[1])
    own_y.start()

    each(1, 2 * n_ep, lambda j: spread(j).wait_send())
    for copy in pair_w:
        copy.wait_send()
    x_sent()
    h_sent()

    own_y.wait()
    each(1, 2 * n_ep, lambda j: got(j).wait_recv())
    y = y_all[...].reshape(n_exp * CAP, width)
    combined = dot(combine_w[0], y, ((1,), (0,))) + dot(combine_w[1], y, ((1,), (0,)))
    norm_all[tp] = jnp.sum((combined * combined).T, axis=0, keepdims=True)

    def tell(j):
        return pltpu.make_async_remote_copy(
            src_ref=norm_all.at[tp], dst_ref=norm_all.at[tp],
            send_sem=n_send.at[j], recv_sem=n_recv.at[j],
            device_id=(ep, (tp + j) % n_tp), device_id_type=MESH,
        )

    def told(j):
        t_from = (tp + n_tp - j) % n_tp
        return pltpu.make_async_remote_copy(
            src_ref=norm_all.at[t_from], dst_ref=norm_all.at[t_from],
            send_sem=n_send.at[j], recv_sem=n_recv.at[j],
            device_id=(ep, t_from), device_id_type=MESH,
        )

    each(1, n_tp, lambda j: tell(j).start())
    scaled = combined * gain_ref[...]
    each(1, 2 * n_ep, lambda j: give(j).wait_send())
    each(1, n_tp, lambda j: told(j).wait_recv())
    total = jnp.sum(norm_all[...], axis=0)
    final_scale = lax.rsqrt(total * (1.0 / features) + NORM_EPS)
    final_scale = jnp.broadcast_to(final_scale, (tok_rows, tok_rows)).T
    out_ref[...] = (scaled * final_scale[:, :width]).astype(out_ref.dtype)
    each(1, n_tp, lambda j: tell(j).wait_send())


def body(tokens, routing, gate_weights, w_gate, w_up, w_down, out_gain):
    n_ep = lax.axis_size("ep")
    n_tp = lax.axis_size("tp")
    n_z = n_tp // 2
    tok_rows, width = tokens.shape
    n_exp = EXP_DEV * n_ep
    rows = n_ep * CAP
    hid, model = w_gate.shape[1], w_gate.shape[2]
    full = w_down.shape[1]
    vmem = pl.BlockSpec(memory_space=pltpu.VMEM)
    hbm = pl.BlockSpec(memory_space=pl.ANY)
    dma = pltpu.SemaphoreType.DMA
    return pl.pallas_call(
        functools.partial(layer_kernel, n_ep, n_z),
        out_shape=jax.ShapeDtypeStruct((tok_rows, width), BF16),
        in_specs=[vmem, vmem, vmem, hbm, hbm, hbm, vmem],
        out_specs=vmem,
        scratch_shapes=[
            pltpu.VMEM((n_exp, CAP, width), BF16),
            pltpu.VMEM((2, tok_rows, n_exp * CAP), BF16),
            pltpu.VMEM((n_z, 2, rows, width), BF16),
            pltpu.VMEM((2, 2, hid, model), BF16),
            pltpu.VMEM((full, 2 * width), BF16),
            pltpu.VMEM((4 * hid, rows), F32),
            pltpu.VMEM((rows, width), F32),
            pltpu.VMEM((n_z, 2, 2 * hid, rows // 2), BF16),
            pltpu.VMEM((2, rows // 2, 2 * width), F32),
            pltpu.VMEM((2, n_ep, CAP, width), BF16),
            pltpu.VMEM((n_exp, CAP, width), BF16),
            pltpu.VMEM((n_tp, 1, tok_rows), F32),
            dma((3,)), dma((3,)), dma((3,)), dma((2 * n_ep,)), dma((2 * n_ep,)), dma((2,)),
            dma((2, n_z // 2, 2)), dma((2, n_z // 2, 2)),
            dma((2, n_z // 2, 2)), dma((2, n_z // 2, 2)),
            dma((2 * n_ep,)), dma((2 * n_ep,)), dma((n_tp,)), dma((n_tp,)),
        ],
        compiler_params=pltpu.CompilerParams(collective_id=0, has_side_effects=True),
        name="expert_layer",
    )(tokens, routing.T, gate_weights.T, w_gate, w_up, w_down, out_gain.reshape(1, -1))


def solution(mesh):
    placed = (
        P("ep", "tp"),
        P("ep", None),
        P("ep", None),
        P("ep", "tp", None),
        P("ep", "tp", None),
        P("ep", None, "tp"),
        P("tp"),
    )
    return jax.shard_map(body, mesh=mesh, in_specs=placed, out_specs=P("ep", "tp"), check_vma=False)
```

```python
import functools
import math
import jax
import jax.numpy as jnp
from jax import lax
from jax.experimental import pallas as pl
from jax.experimental.pallas import tpu as pltpu
from jax.sharding import PartitionSpec as P

EXP_DEV = 2
CAP = 32
NORM_EPS = 1e-05
MESH = pl.DeviceIdType.MESH
F32 = jnp.float32
BF16 = jnp.bfloat16


def dot(a, b, dims):
    return lax.dot_general(a, b, (dims, ((), ())), preferred_element_type=F32)


def layer_kernel(
    side, n_z, tok_ref, rt_ref, gw_ref, wg_ref, wu_ref, wd_ref, gain_ref, out_ref,
    t_all, routes, gates, gain, select, staged, combine_w, x_all, w_all, d_all, acc, squares,
    h_all, o_acc, back, y_all, norm_all,
    in_sem, w_sem, w_send, w_recv, m_send, m_recv, q_send, q_recv, t_send, t_recv, p_send, p_recv,
    h_send, h_recv, r_send, r_recv, n_send, n_recv, local_sem,
):
    ep = lax.axis_index("ep")
    tp = lax.axis_index("tp")
    z, c = tp // 2, tp % 2
    y, x = ep // side, ep % side
    other = 1 - c
    partner = 2 * z + other
    above, below = (z + 1) % n_z, (z + n_z - 1) % n_z
    n_ep = side * side
    n_exp = EXP_DEV * n_ep
    n_tp = 2 * n_z
    width = tok_ref.shape[1]
    tok_rows = tok_ref.shape[0]
    half = n_z // 2
    rows = n_ep * CAP

    g_own = other * y + c * x
    d_own = other * x + c * y

    def g_ep(g):
        return other * (g * side + x) + c * (y * side + g)

    def d_ep(d):
        return other * (y * side + d) + c * (d * side + x)

    def each(lo, hi, act):
        def step(j, carry):
            act(j)
            return carry

        lax.fori_loop(lo, hi, step, 0)

    barrier = pltpu.get_barrier_semaphore()

    def greet(p_to, t_to):
        pl.semaphore_signal(barrier, inc=1, device_id=(p_to, t_to), device_id_type=MESH)

    for k in range(1, side):
        greet(g_ep((g_own + k) % side), tp)
        greet(y * side + (x + k) % side, 2 * z)
        greet(((y + k) % side) * side + x, 2 * z + 1)
    greet(ep, partner)
    greet(ep, 2 * above + c)
    greet(ep, 2 * below + c)
    n_greet = 3 * (side - 1) + 3

    own_in = [
        pltpu.make_async_copy(tok_ref, t_all.at[z, g_own // 2, g_own % 2], in_sem.at[0]),
        pltpu.make_async_copy(rt_ref, routes.at[g_own], in_sem.at[1]),
        pltpu.make_async_copy(gw_ref, gates, in_sem.at[2]),
        pltpu.make_async_copy(gain_ref, gain, in_sem.at[3]),
    ]
    own_w = [
        pltpu.make_async_copy(wg_ref.at[c], w_all.at[0, c], w_sem.at[0]),
        pltpu.make_async_copy(wu_ref.at[c], w_all.at[1, c], w_sem.at[1]),
        pltpu.make_async_copy(wd_ref.at[c], d_all.at[:, pl.ds(pl.multiple_of(c * width, width), width)], w_sem.at[2]),
    ]
    for copy in own_in:
        copy.start()
    for copy in own_w:
        copy.start()
    own_in[0].wait()
    own_in[1].wait()
    pl.semaphore_wait(barrier, n_greet)

    def share(k):
        to = (g_ep((g_own + k) % side), tp)
        mine = t_all.at[z, g_own // 2, g_own % 2]
        return [
            pltpu.make_async_remote_copy(
                src_ref=mine, dst_ref=mine, send_sem=m_send.at[k - 1], recv_sem=m_recv.at[k - 1],
                device_id=to, device_id_type=MESH,
            ),
            pltpu.make_async_remote_copy(
                src_ref=routes.at[g_own], dst_ref=routes.at[g_own],
                send_sem=q_send.at[k - 1], recv_sem=q_recv.at[k - 1],
                device_id=to, device_id_type=MESH,
            ),
        ]

    def shared(k):
        g = (g_own + side - k) % side
        theirs = t_all.at[z, g // 2, g % 2]
        return [
            pltpu.make_async_remote_copy(
                src_ref=theirs, dst_ref=theirs, send_sem=m_send.at[k - 1], recv_sem=m_recv.at[k - 1],
                device_id=(g_ep(g), tp), device_id_type=MESH,
            ),
            pltpu.make_async_remote_copy(
                src_ref=routes.at[g], dst_ref=routes.at[g],
                send_sem=q_send.at[k - 1], recv_sem=q_recv.at[k - 1],
                device_id=(g_ep(g), tp), device_id_type=MESH,
            ),
        ]

    for k in (2, 1, 3):
        for copy in share(k):
            copy.start()

    def pair(i, src, dst):
        return pltpu.make_async_remote_copy(
            src_ref=src, dst_ref=dst, send_sem=w_send.at[i], recv_sem=w_recv.at[i],
            device_id=(ep, partner), device_id_type=MESH,
        )

    def d_part(k):
        return d_all.at[:, pl.ds(pl.multiple_of(k * width, width), width)]

    pair_w = [
        pair(0, wg_ref.at[other], w_all.at[0, c]),
        pair(1, wu_ref.at[other], w_all.at[1, c]),
        pair(2, wd_ref.at[other], d_part(c)),
    ]
    pair_in = [
        pair(0, wg_ref.at[other], w_all.at[0, other]),
        pair(1, wu_ref.at[other], w_all.at[1, other]),
        pair(2, wd_ref.at[other], d_part(other)),
    ]
    for copy in pair_w:
        copy.start()

    acc[...] = jnp.zeros_like(acc)
    squares[...] = jnp.zeros_like(squares)
    o_acc[...] = jnp.zeros_like(o_acc)

    earlier = jnp.where(
        lax.broadcasted_iota(jnp.int32, (tok_rows, tok_rows), 0)
        < lax.broadcasted_iota(jnp.int32, (tok_rows, tok_rows), 1),
        1.0, 0.0,
    ).astype(BF16)

    def slots(hit):
        rank = dot(jnp.where(hit, 1.0, 0.0).astype(BF16), earlier, ((1,), (0,)))
        rank = jnp.where(hit, rank, -1.0)
        slot_ids = lax.broadcasted_iota(jnp.int32, (hit.shape[0], CAP, tok_rows), 1).astype(F32)
        return slot_ids == rank[:, None, :]

    def hits_of(ids, route):
        return [ids == route[k : k + 1, :] for k in range(route.shape[0])]

    order = ((0, 0), (1, 1), (0, 1), (1, 0))

    def block_of(way, s):
        return (z + n_z - s) % n_z if way == 0 else (z + s) % n_z

    def hop(buf, send, recv, way, s, ch):
        block = block_of(way, s)
        return pltpu.make_async_remote_copy(
            src_ref=buf.at[block, ch], dst_ref=buf.at[block, ch],
            send_sem=send.at[way, s, ch], recv_sem=recv.at[way, s, ch],
            device_id=(ep, 2 * (above if way == 0 else below) + c), device_id_type=MESH,
        )

    def came(buf, send, recv, way, s, ch):
        block = block_of(way, s)
        return pltpu.make_async_remote_copy(
            src_ref=buf.at[block, ch], dst_ref=buf.at[block, ch],
            send_sem=send.at[way, s - 1, ch], recv_sem=recv.at[way, s - 1, ch],
            device_id=(ep, 2 * (below if way == 0 else above) + c), device_id_type=MESH,
        )

    def ring_start(ring):
        for way, ch in order:
            hop(*ring, way, 0, ch).start()

    def ring_step(ring, s):
        for way, ch in order:
            came(*ring, way, s, ch).wait_recv()
            hop(*ring, way, s, ch).start()

    def ring_late(ring):
        s = half - 1
        for way, ch in order:
            came(*ring, way, s, ch).wait_recv()
            if way == ch:
                hop(*ring, way, s, ch).start()

    def ring_sent(ring):
        def done(s):
            for way, ch in order:
                hop(*ring, way, s, ch).wait_send()

        each(0, half - 1, done)
        for way in (0, 1):
            hop(*ring, way, half - 1, way).wait_send()

    t_ring = (t_all, t_send, t_recv)
    h_ring = (h_all, h_send, h_recv)

    for k in (1, 3, 2):
        for copy in shared(k):
            copy.wait_recv()
    ring_start(t_ring)

    line = lax.broadcasted_iota(jnp.int32, (2 * side, tok_rows), 0)
    line = 2 * d_ep(line // 2) + line % 2
    line_hits = [functools.reduce(jnp.logical_or, hits_of(line, routes[g])) for g in range(side)]
    chosen = slots(jnp.concatenate([jnp.where(h, 1.0, 0.0) for h in line_hits], axis=0) > 0.5)
    select[...] = jnp.where(chosen, 1.0, 0.0).astype(BF16).reshape(side, 2 * side * CAP, tok_rows)

    def piece(block, d, e):
        return pltpu.make_async_remote_copy(
            src_ref=staged.at[block, 2 * d + e], dst_ref=x_all.at[block, c, d_own],
            send_sem=p_send.at[block, 2 * d + e], recv_sem=p_recv.at[block, c, d_own],
            device_id=(d_ep(d), 2 * z + e), device_id_type=MESH,
        )

    def own_piece(block):
        return pltpu.make_async_copy(
            staged.at[block, 2 * d_own + c], x_all.at[block, c, d_own], p_recv.at[block, c, d_own]
        )

    def expand(block):
        for g in range(side):
            picked = dot(select[g], t_all[block, g // 2, g % 2], ((1,), (0,))).astype(BF16)
            staged[block, :, g] = picked.reshape(2 * side, CAP, width)
        for k in (2, 1, 3):
            for e in range(2):
                piece(block, (d_own + k) % side, e).start()
        piece(block, d_own, other).start()
        own_piece(block).start()

    def pieces_sent(block):
        for k in range(1, side):
            for e in range(2):
                piece(block, (d_own + k) % side, e).wait_send()
        piece(block, d_own, other).wait_send()

    n_hid = 2 * w_all.shape[2]

    def project(block):
        for ch in range(2):
            for i in range(side):
                pltpu.make_async_copy(
                    staged.at[block, 0], x_all.at[block, ch, i], p_recv.at[block, ch, i]
                ).wait()
            parts = [
                x_all[block, ch, i, j] if ch == 0 else x_all[block, ch, j, i]
                for i in range(side) for j in range(side)
            ]
            data = jnp.concatenate(parts, axis=0)
            column = pl.multiple_of((2 * block + ch) * width, width)
            w = w_all[:, :, :, pl.ds(column, width)].reshape(2 * n_hid, width)
            acc[...] += dot(w, data, ((1,), (1,)))
            data = data.astype(F32)
            squares[...] += data * data

    expand(z)
    for copy in own_w:
        copy.wait()
    for copy in pair_in:
        copy.wait_recv()

    def middle(s):
        ring_step(t_ring, s)
        for way in range(2):
            expand(block_of(way, s))

        @pl.when(s >= 3)
        def _():
            for way in range(2):
                project(block_of(way, s - 2))

    each(1, half - 1, middle)
    ring_late(t_ring)
    for way in range(2):
        expand(block_of(way, half - 1))
    for way in range(2):
        project(block_of(way, half - 3))
    for way in range(2):
        came(*t_ring, way, half, way).wait_recv()
    expand(block_of(0, half))
    project(z)
    for way in range(2):
        project(block_of(way, half - 2))

    own_in[2].wait()
    own_in[3].wait()
    all_ids = lax.broadcasted_iota(jnp.int32, (n_exp, tok_rows), 0)
    hits = hits_of(all_ids, routes[g_own])
    gate_of = functools.reduce(jnp.add, [jnp.where(h, gates[k : k + 1, :], 0.0) for k, h in enumerate(hits)])
    weight = jnp.where(slots(functools.reduce(jnp.logical_or, hits)), gate_of[:, None, :], 0.0)
    weight = weight.reshape(n_exp * CAP, tok_rows).T
    weight_hi = weight.astype(BF16)
    combine_w[0] = weight_hi
    combine_w[1] = (weight - weight_hi.astype(F32)).astype(BF16)

    for way in range(2):
        project(block_of(way, half - 1))
    project(block_of(0, half))

    features = n_tp * width
    square_sum = jnp.sum(squares[...].T, axis=0, keepdims=True)
    row_scale = lax.rsqrt(square_sum * (1.0 / features) + NORM_EPS)
    gate = acc[0:n_hid, :] * row_scale
    up = acc[n_hid : 2 * n_hid, :] * row_scale
    hidden = (gate / (1.0 + jnp.exp(-gate)) * up).astype(BF16)
    part = rows // 2
    for i in range(2):
        h_all[z, i] = hidden[:, i * part : (i + 1) * part]

    def down(block, ch):
        w = d_all[pl.ds(pl.multiple_of(block * n_hid, n_hid), n_hid), :]
        o_acc[ch] += dot(h_all[block, ch], w, ((0,), (0,)))

    ring_start(h_ring)
    for ch in range(2):
        down(z, ch)

    def h_middle(s):
        ring_step(h_ring, s)
        for way, ch in order:
            down(block_of(way, s), ch)

    each(1, half - 1, h_middle)
    ring_late(h_ring)
    for way, ch in order:
        down(block_of(way, half - 1), ch)
    for way in range(2):
        came(*h_ring, way, half, way).wait_recv()
        down(block_of(way, half), way)

    s_half = side // 2
    for i in range(2):
        for h in range(2):
            back[h, i * s_half : (i + 1) * s_half] = (
                o_acc[i, :, h * width : (h + 1) * width].astype(BF16).reshape(s_half, side, CAP, width)
            )

    def give(j):
        p_to, c_to = (ep + j // 2) % n_ep, (c + j % 2) % 2
        return pltpu.make_async_remote_copy(
            src_ref=back.at[c_to, p_to % side, p_to // side], dst_ref=y_all.at[2 * ep + c],
            send_sem=r_send.at[j], recv_sem=r_recv.at[j],
            device_id=(p_to, 2 * z + c_to), device_id_type=MESH,
        )

    def got(j):
        p_from, c_from = (ep + n_ep - j // 2) % n_ep, (c + j % 2) % 2
        return pltpu.make_async_remote_copy(
            src_ref=back.at[0, 0, 0], dst_ref=y_all.at[2 * p_from + c_from],
            send_sem=r_send.at[j], recv_sem=r_recv.at[j],
            device_id=(p_from, 2 * z + c_from), device_id_type=MESH,
        )

    each(1, 2 * n_ep, lambda j: give(j).start())
    own_y = pltpu.make_async_copy(back.at[c, ep % side, ep // side], y_all.at[2 * ep + c], local_sem.at[0])
    own_y.start()

    for k in range(1, side):
        for copy in share(k):
            copy.wait_send()
    for copy in pair_w:
        copy.wait_send()
    ring_sent(t_ring)
    each(0, n_z, pieces_sent)
    ring_sent(h_ring)

    own_y.wait()
    each(1, 2 * n_ep, lambda j: got(j).wait_recv())
    returned = y_all[...].reshape(n_exp * CAP, width)
    combined = dot(combine_w[0], returned, ((1,), (0,))) + dot(combine_w[1], returned, ((1,), (0,)))
    norm_all[tp] = jnp.sum((combined * combined).T, axis=0, keepdims=True)

    def tell(j):
        return pltpu.make_async_remote_copy(
            src_ref=norm_all.at[tp], dst_ref=norm_all.at[tp],
            send_sem=n_send.at[j], recv_sem=n_recv.at[j],
            device_id=(ep, (tp + j) % n_tp), device_id_type=MESH,
        )

    def told(j):
        t_from = (tp + n_tp - j) % n_tp
        return pltpu.make_async_remote_copy(
            src_ref=norm_all.at[t_from], dst_ref=norm_all.at[t_from],
            send_sem=n_send.at[j], recv_sem=n_recv.at[j],
            device_id=(ep, t_from), device_id_type=MESH,
        )

    each(1, n_tp, lambda j: tell(j).start())
    scaled = combined * gain[...]
    each(1, 2 * n_ep, lambda j: give(j).wait_send())
    each(1, n_tp, lambda j: told(j).wait_recv())
    total = jnp.sum(norm_all[...], axis=0)
    final_scale = lax.rsqrt(total * (1.0 / features) + NORM_EPS)
    final_scale = jnp.broadcast_to(final_scale, (tok_rows, tok_rows)).T
    out_ref[...] = (scaled * final_scale[:, :width]).astype(out_ref.dtype)
    each(1, n_tp, lambda j: tell(j).wait_send())


def body(tokens, routing, gate_weights, w_gate, w_up, w_down, out_gain):
    n_ep = lax.axis_size("ep")
    n_tp = lax.axis_size("tp")
    side = math.isqrt(n_ep)
    n_z = n_tp // 2
    tok_rows, width = tokens.shape
    top = routing.shape[1]
    n_exp = EXP_DEV * n_ep
    rows = n_ep * CAP
    hid, model = w_gate.shape[1], w_gate.shape[2]
    full = w_down.shape[1]
    hbm = pl.BlockSpec(memory_space=pl.ANY)
    dma = pltpu.SemaphoreType.DMA
    ring = (2, n_z // 2, 2)
    return pl.pallas_call(
        functools.partial(layer_kernel, side, n_z),
        out_shape=jax.ShapeDtypeStruct((tok_rows, width), BF16),
        in_specs=[hbm] * 7,
        out_specs=pl.BlockSpec(memory_space=pltpu.VMEM),
        scratch_shapes=[
            pltpu.VMEM((n_z, side // 2, 2, tok_rows, width), BF16),
            pltpu.VMEM((side, top, tok_rows), jnp.int32),
            pltpu.VMEM((top, tok_rows), F32),
            pltpu.VMEM((1, width), F32),
            pltpu.VMEM((side, 2 * side * CAP, tok_rows), BF16),
            pltpu.VMEM((n_z, 2 * side, side, CAP, width), BF16),
            pltpu.VMEM((2, tok_rows, n_exp * CAP), BF16),
            pltpu.VMEM((n_z, 2, side, side, CAP, width), BF16),
            pltpu.VMEM((2, 2, hid, model), BF16),
            pltpu.VMEM((full, 2 * width), BF16),
            pltpu.VMEM((4 * hid, rows), F32),
            pltpu.VMEM((rows, width), F32),
            pltpu.VMEM((n_z, 2, 2 * hid, rows // 2), BF16),
            pltpu.VMEM((2, rows // 2, 2 * width), F32),
            pltpu.VMEM((2, side, side, CAP, width), BF16),
            pltpu.VMEM((n_exp, CAP, width), BF16),
            pltpu.VMEM((n_tp, 1, tok_rows), F32),
            dma((4,)), dma((3,)), dma((3,)), dma((3,)),
            dma((side - 1,)), dma((side - 1,)), dma((side - 1,)), dma((side - 1,)),
            dma(ring), dma(ring), dma((n_z, 2 * side)), dma((n_z, 2, side)),
            dma(ring), dma(ring), dma((2 * n_ep,)), dma((2 * n_ep,)), dma((n_tp,)), dma((n_tp,)), dma((1,)),
        ],
        compiler_params=pltpu.CompilerParams(collective_id=0, has_side_effects=True),
        name="expert_layer",
    )(tokens, routing.T, gate_weights.T, w_gate, w_up, w_down, out_gain.reshape(1, -1))


def solution(mesh):
    placed = (
        P("ep", "tp"),
        P("ep", None),
        P("ep", None),
        P("ep", "tp", None),
        P("ep", "tp", None),
        P("ep", None, "tp"),
        P("tp"),
    )
    return jax.shard_map(body, mesh=mesh, in_specs=placed, out_specs=P("ep", "tp"), check_vma=False)
```
